32 devices in a mesh: sp: 8 (over z, x), tp: 4 (over y, core).
Axes of the slice: x: 2, y: 2, z: 4, core: 2. Of those that a mesh axis runs over, the one named last changes fastest.
Arguments:
- queries: bfloat16 [1024, 32, 128], P('sp', 'tp'), may hold values from -6 to 6
- keys: bfloat16 [1024, 8, 128], P('sp', 'tp'), may hold values from -6 to 6
- values: bfloat16 [1024, 8, 128], P('sp', 'tp'), may hold values from -6 to 6
- q_gain: float32 [128], replicated, may hold values from 0.2 to 8
- k_gain: float32 [128], replicated, may hold values from 0.2 to 8
- w_out: bfloat16 [4096, 2048], P('tp'), may hold values from -0.09375 to 0.09375
- residual: bfloat16 [1024, 2048], P(('sp', 'tp')), may hold values from -6 to 6
- gain_mix: float32 [2048], replicated, may hold values from 0.1 to 1.9
- gain_pre: float32 [2048], replicated, may hold values from 0.1 to 1.9
- routes: int32 [1024, 4], P(('sp', 'tp')), may hold values from 0 to 7, all different within a row; in each aligned block of 32 rows (0 to 31, 32 to 63, ...) at most 32 rows name the same one
- route_weights: float32 [1024, 4], P(('sp', 'tp')), may hold values from 0.1 to 1
- w_gate: bfloat16 [8, 2048, 2048], P('sp', None, 'tp'), may hold values from -0.5 to 0.5
- w_up: bfloat16 [8, 2048, 2048], P('sp', None, 'tp'), may hold values from -0.5 to 0.5
- w_down: bfloat16 [8, 2048, 2048], P('sp', 'tp'), may hold values from -0.125 to 0.125
- gain_moe: float32 [2048], replicated, may hold values from 0.1 to 1.9
Outputs:
- layer_out: bfloat16 [1024, 2048], P(('sp', 'tp'))
The draws below stay inside these ranges and needn't reach their ends.
Inputs may be any that keep to these rules, and one draw needn't show every extreme that they name: `routes`: each row names 4 different experts. In each aligned block of 32 rows (the rows of one device) no expert is named by more than 32 rows, a bound that some block reaches.
All inputs are finite; a program needn't handle non-finite values.
Results may differ from the reference program's by a relative error of at most 0.017.
The reference program's roundings to bfloat16 on the way count: a program that leaves them out, or rounds other values in their place, can miss the bound.
Values may be sent and summed in bfloat16 or wider, within the bound.
A program may use at most 128 MiB of HBM per device.

```python
import math
import jax
import jax.numpy as jnp
import numpy as np
from jax import lax

D = 2048
Q_HEADS = 32
KV_HEADS = 8
HD = 128
FF = 2048
TOP = 4
GRID_W = 64
TOKENS = 1024
TOK_TP = 32
EXPERTS = 8
CAP = 32
N_TP = 4


def gain_draw(key):
    return 1.0 + 0.18 * jax.random.truncated_normal(key, -4.0, 4.0, (HD,), jnp.float32)


def draw_q_gain(key, part):
    return gain_draw(jax.random.fold_in(key, 31))


def draw_k_gain(key, part):
    return gain_draw(jax.random.fold_in(key, 57))


def steps_of(own_key, shape, shards, least, high):
    def one(position, blocks):
        draws = jax.random.uniform(jax.random.fold_in(jax.random.fold_in(own_key, 6), position), (blocks,), jnp.float32, least / len(shards), high / len(shards))
        return jnp.repeat(jnp.exp(draws), shape[position] // blocks).reshape((-1,) + (1,) * (len(shape) - position - 1))

    loudness = one(*shards[0])
    for cut in shards[1:]:
        loudness = loudness * one(*cut)
    return loudness


def routed_block(stream_key, own, number, rows, number_of, top, bound, lean):
    order = jax.random.permutation(stream_key, number_of)
    packed, common = shares(number_of, rows * top, bound, lean, True), shares(number_of, rows * top, bound, lean, False)
    places = jnp.arange(number_of)

    def named(lengths, rotation):
        used = int((lengths > 0).sum())
        fixed = max(1, used // 4)
        shifted = fixed + (places - fixed + rotation * (used - fixed)) % max(1, number_of - fixed)
        return jnp.zeros((number_of,), jnp.int32).at[order[jnp.where(places < fixed, places, shifted)]].set(jnp.asarray(lengths, jnp.int32))

    lengths = jnp.where(number % 4 == 0, named(packed, number // 4), named(common, number - number // 4 - 1))
    mixed = jax.random.permutation(jax.random.fold_in(own, 3), number_of)
    donor, taker = mixed[0:number_of // 2 * 2:2], mixed[1:number_of // 2 * 2:2]
    room = jnp.minimum(lengths[donor] - 1, bound - lengths[taker]) // 2
    room = jnp.where((donor == order[0]) | (taker == order[0]) | (lengths[taker] == 0), 0, jnp.maximum(room, 0))
    shifted = jax.random.randint(jax.random.fold_in(own, 4), (number_of // 2,), 0, 1 << 20) % (room + 1)
    lengths = lengths.at[donor].add(-shifted).at[taker].add(shifted)
    members = jnp.searchsorted(jnp.cumsum(lengths), jnp.arange(rows * top), side="right").astype(jnp.int32)
    listing = members.reshape(top, rows).T
    listing = listing[jax.random.permutation(jax.random.fold_in(own, 1), rows)]
    rotation = jax.random.randint(jax.random.fold_in(own, 2), (rows, 1), 0, top)
    return jnp.take_along_axis(listing, (jnp.arange(top)[None, :] + rotation) % top, axis=1)


def shares(amount, total, limit, lean, full):
    portions = [(1 << 20) // math.isqrt(standing ** lean) + 1 for standing in range(1, amount + 1)]
    largest = limit if full else min(limit, max(-(-total // amount), total * portions[0] // sum(portions)))
    least = 1 if total - largest >= amount - 1 else 0
    given, spare = [largest] + [least] * (amount - 1), total - largest - least * (amount - 1)
    while spare > 0:
        free = [i for i in range(1, amount) if given[i] < largest] or [i for i in range(1, amount) if given[i] < limit]
        mass, remaining = sum([portions[i] for i in free]), spare
        for i in free:
            addition = min(limit - given[i], max(1, remaining * portions[i] // mass), spare)
            given[i] = given[i] + addition
            spare = spare - addition
    return np.array(given)


def normal_values(stream_key, dims, spread, limit, shards=(), kind=jnp.bfloat16):
    loudness = steps_of(stream_key, dims, shards, -0.22, 0.18) if shards else 1.0
    values = jax.random.normal(stream_key, dims, jnp.float32) * spread * loudness
    return jnp.minimum(jnp.maximum(values, -limit), limit).astype(kind)


def setup_inputs(seed: int = 0) -> dict:
    key_of = jax.random.split(jax.random.key(seed), 16)
    queries = normal_values(key_of[0], (TOKENS, Q_HEADS, HD), 1.0, 6.0, ((0, 8), (1, 4)))
    keys = normal_values(key_of[1], (TOKENS, KV_HEADS, HD), 1.0, 6.0, ((0, 8), (1, 4)))
    values = normal_values(key_of[2], (TOKENS, KV_HEADS, HD), 1.0, 6.0, ((0, 8), (1, 4)))
    q_gain = draw_q_gain(jax.random.fold_in(key_of[15], 71), 0)
    k_gain = draw_k_gain(jax.random.fold_in(key_of[15], 71), 0)
    w_out = normal_values(key_of[5], (Q_HEADS * HD, D), (Q_HEADS * HD) ** -0.5, 0.09375, ((0, 4),))
    residual = normal_values(key_of[6], (TOKENS, D), 1.0, 6.0, ((0, 32),))
    gain_mix = jnp.clip(1.0 + 0.18 * jax.random.normal(key_of[7], (D,), jnp.float32), 0.1, 1.9)
    gain_pre = jnp.clip(1.0 + 0.18 * jax.random.normal(key_of[8], (D,), jnp.float32), 0.1, 1.9)
    routes_keys = jax.random.split(jax.random.fold_in(key_of[9], 1), TOKENS // TOK_TP)
    routes_turns = jax.random.permutation(jax.random.fold_in(key_of[9], 3), TOKENS // TOK_TP)
    routes = jax.vmap(lambda own, number: routed_block(jax.random.fold_in(key_of[9], 2), own, number, TOK_TP, EXPERTS, TOP, CAP, 1))(routes_keys, routes_turns).reshape((TOKENS, TOP))
    route_weights = jnp.clip(jnp.exp(math.log(1.0) - 2.3025851 * jax.random.uniform(key_of[10], (TOKENS, TOP), jnp.float32) ** steps_of(key_of[10], (TOKENS, TOP), ((0, 32),), -0.2, 0.2)), 0.1, 1.0)
    w_gate = normal_values(key_of[11], (EXPERTS, D, FF), (D // 16) ** -0.5, 0.5, ((0, 8), (2, 4)))
    w_up = normal_values(key_of[12], (EXPERTS, D, FF), (D // 16) ** -0.5, 0.5, ((0, 8), (2, 4)))
    w_down = normal_values(key_of[13], (EXPERTS, FF, D), FF ** -0.5, 0.125, ((0, 8), (1, 4)))
    gain_moe = jnp.clip(1.0 + 0.18 * jax.random.normal(key_of[14], (D,), jnp.float32), 0.1, 1.9)
    return {"queries": queries, "keys": keys, "values": values, "q_gain": q_gain, "k_gain": k_gain, "w_out": w_out, "residual": residual, "gain_mix": gain_mix, "gain_pre": gain_pre, "routes": routes, "route_weights": route_weights, "w_gate": w_gate, "w_up": w_up, "w_down": w_down, "gain_moe": gain_moe}


norm_eps = 1e-06
rope_theta = 10000.0
clamp_limit = 7.0
swish_alpha = 1.702

def rope_tables(positions, head_size):
    row_index = (positions // GRID_W).astype(jnp.float32)
    col_index = (positions % GRID_W).astype(jnp.float32)
    freq_count = head_size // 4
    inverse = rope_theta ** (-jnp.arange(freq_count, dtype=jnp.float32) / freq_count)
    angles = jnp.stack([row_index[:, None] * inverse, col_index[:, None] * inverse], axis=1)
    return (jnp.cos(angles), jnp.sin(angles))

def turn(array_in, cosine_table, sine_table):
    token_count, head_count, head_size = array_in.shape
    split_field = array_in.reshape(token_count, head_count, 2, 2, head_size // 4)
    first_half = split_field[:, :, :, 0, :]
    second_half = split_field[:, :, :, 1, :]
    cos_wide = cosine_table[:, None]
    sin_wide = sine_table[:, None]
    turned = jnp.stack([first_half * cos_wide - second_half * sin_wide, second_half * cos_wide + first_half * sin_wide], axis=3)
    return turned.reshape(token_count, head_count, head_size)

def scale_rows(array_in, gain_vec):
    return array_in * lax.rsqrt(lax.optimization_barrier(jnp.mean(array_in * array_in, axis=-1, keepdims=True)) + norm_eps) * gain_vec

def reference(queries, keys, values, q_gain, k_gain, w_out, residual, gain_mix, gain_pre, routes, route_weights, w_gate, w_up, w_down, gain_moe):
    positions = jnp.arange(TOKENS, dtype=jnp.int32)
    cosine_table, sine_table = rope_tables(positions, HD)
    q_turned = (turn(scale_rows(queries.astype(jnp.float32), q_gain), cosine_table, sine_table) * HD ** (-0.5)).astype(jnp.bfloat16)
    k_turned = turn(scale_rows(keys.astype(jnp.float32), k_gain), cosine_table, sine_table).astype(jnp.bfloat16)
    group_size = Q_HEADS // KV_HEADS
    qblock = math.gcd(TOKENS, 512)
    blocks = q_turned.reshape(TOKENS // qblock, qblock, KV_HEADS, group_size, HD)
    k_wide = k_turned.astype(jnp.float32)
    v_wide = values.astype(jnp.float32)

    def attend(block):
        scores = jnp.einsum('qkgd,skd->kgqs', block.astype(jnp.float32), k_wide)
        unnorm = jnp.exp(scores - lax.optimization_barrier(jnp.max(scores, axis=-1, keepdims=True)))
        totals = lax.optimization_barrier(jnp.sum(unnorm, axis=-1))
        summed = jnp.einsum('kgqs,skd->qkgd', unnorm.astype(jnp.bfloat16).astype(jnp.float32), v_wide)
        return (summed / jnp.moveaxis(totals, 2, 0)[..., None]).astype(jnp.bfloat16)
    mixed_heads = lax.map(attend, blocks).reshape(TOKENS, Q_HEADS * HD)
    projected = jnp.dot(mixed_heads, w_out, preferred_element_type=jnp.float32)
    middle = residual.astype(jnp.float32) + scale_rows(projected, gain_mix)
    normed = scale_rows(middle, gain_pre).astype(jnp.bfloat16)
    block_count = TOKENS // TOK_TP
    assign = TOK_TP * TOP
    flat_routes = routes.reshape(block_count, assign)
    expert_hits = (flat_routes[:, :, None] == jnp.arange(EXPERTS, dtype=jnp.int32)[None, None, :]).astype(jnp.int32)
    slot_index = lax.optimization_barrier(jnp.sum((jnp.cumsum(expert_hits, axis=1) - expert_hits) * expert_hits, axis=2)).astype(jnp.int32)
    block_ids = jnp.broadcast_to(jnp.arange(block_count, dtype=jnp.int32)[:, None], (block_count, assign))
    token_ids = (block_ids * TOK_TP + jnp.arange(assign, dtype=jnp.int32)[None, :] // TOP).astype(jnp.int32)
    slot_tokens = jnp.full((EXPERTS, block_count, CAP), TOKENS, jnp.int32).at[flat_routes, block_ids, slot_index].set(token_ids)
    padded = jnp.concatenate([normed, jnp.zeros((1, D), jnp.bfloat16)], axis=0)
    group_width = FF // N_TP

    def serve_expert(expert_args):
        token_rows, gate_weight, up_weight, down_weight = expert_args
        arrived_rows = padded[token_rows.reshape(-1)]
        gate_pre = jnp.minimum(jnp.dot(arrived_rows, gate_weight, preferred_element_type=jnp.float32), clamp_limit)
        up_pre = jnp.clip(jnp.dot(arrived_rows, up_weight, preferred_element_type=jnp.float32), -clamp_limit, clamp_limit)
        active = (gate_pre * jax.nn.sigmoid(swish_alpha * gate_pre) * (up_pre + 1.0)).astype(jnp.bfloat16)
        group_sums = jnp.einsum('rqf,qfd->rqd', active.reshape(-1, N_TP, group_width).astype(jnp.float32), down_weight.reshape(N_TP, group_width, D).astype(jnp.float32))
        group_sums = lax.optimization_barrier(group_sums.astype(jnp.bfloat16)).astype(jnp.float32)
        return lax.optimization_barrier(jnp.sum(group_sums, axis=1)).astype(jnp.bfloat16)
    expert_out = lax.map(serve_expert, (slot_tokens, w_gate, w_up, w_down))
    picked = expert_out.reshape(EXPERTS, block_count, CAP, D)[flat_routes, block_ids, slot_index]
    picked = picked.reshape(TOKENS, TOP, D).astype(jnp.float32)
    mixture = lax.optimization_barrier(jnp.sum(picked * route_weights[:, :, None], axis=1))
    return (middle + scale_rows(mixture, gain_moe)).astype(jnp.bfloat16)
```

```python
import functools
import math

import jax
import jax.numpy as jnp
from jax import lax
from jax.experimental import pallas as pl
from jax.experimental.pallas import tpu as pltpu
from jax.sharding import PartitionSpec as P

TOP = 4
GRID_W = 64


norm_eps = 1e-06
rope_theta = 10000.0
clamp_limit = 7.0
swish_alpha = 1.702


def rope_tables(positions, head_size):
    row_index = (positions // GRID_W).astype(jnp.float32)
    col_index = (positions % GRID_W).astype(jnp.float32)
    freq_count = head_size // 4
    inverse = rope_theta ** (-jnp.arange(freq_count, dtype=jnp.float32) / freq_count)
    angles = jnp.stack([row_index[:, None] * inverse, col_index[:, None] * inverse], axis=1)
    return (jnp.cos(angles), jnp.sin(angles))


def turn(array_in, cosine_table, sine_table):
    token_count, head_count, head_size = array_in.shape
    split_field = array_in.reshape(token_count, head_count, 2, 2, head_size // 4)
    first_half = split_field[:, :, :, 0, :]
    second_half = split_field[:, :, :, 1, :]
    cos_wide = cosine_table[:, None]
    sin_wide = sine_table[:, None]
    turned = jnp.stack(
        [
            first_half * cos_wide - second_half * sin_wide,
            second_half * cos_wide + first_half * sin_wide,
        ],
        axis=3,
    )
    return turned.reshape(token_count, head_count, head_size)


def scale_rows(array_in, gain_vec):
    return (
        array_in
        * lax.rsqrt(jnp.mean(array_in * array_in, axis=-1, keepdims=True) + norm_eps)
        * gain_vec
    )


def slot_table(route_rows, experts, capacity):
    flat_routes = route_rows.reshape(-1)
    expert_hits = (flat_routes[:, None] == jnp.arange(experts, dtype=jnp.int32)[None, :]).astype(
        jnp.int32
    )
    slot_index = jnp.sum((jnp.cumsum(expert_hits, axis=0) - expert_hits) * expert_hits, axis=1)
    target = flat_routes * capacity + slot_index
    slot_onehot = target[:, None] == jnp.arange(experts * capacity, dtype=jnp.int32)[None, :]
    return slot_onehot.astype(jnp.bfloat16).reshape(
        route_rows.shape[0], route_rows.shape[1], experts * capacity
    )


def expert_apply(arrived_rows, w_gate, w_up, w_down):
    gate_pre = jnp.minimum(
        jnp.einsum("serd,edf->serf", arrived_rows, w_gate, preferred_element_type=jnp.float32),
        clamp_limit,
    )
    up_pre = jnp.clip(
        jnp.einsum("serd,edf->serf", arrived_rows, w_up, preferred_element_type=jnp.float32),
        -clamp_limit,
        clamp_limit,
    )
    active = (gate_pre * jax.nn.sigmoid(swish_alpha * gate_pre) * (up_pre + 1.0)).astype(
        jnp.bfloat16
    )
    partial_value = jnp.einsum("serf,efd->serd", active, w_down, preferred_element_type=jnp.float32)
    return lax.optimization_barrier(partial_value.astype(jnp.bfloat16)).astype(jnp.float32)


def send_back(finished):
    return lax.all_to_all(finished, "sp", split_axis=0, concat_axis=0, tiled=True)


MESH = pl.DeviceIdType.MESH
RING = 4
PAIR = 2
LANES = 128


def gather_kernel(n, own_ref, out_ref, send_sem, recv_sem, own_sem):
    me = lax.axis_index("sp")
    tp = lax.axis_index("tp")
    barrier = pltpu.get_barrier_semaphore()

    def greet(i, carry):
        pl.semaphore_signal(
            barrier, inc=1, device_id=(lax.rem(me + i, n), tp), device_id_type=MESH
        )
        return carry

    lax.fori_loop(1, n, greet, 0)
    keep = pltpu.make_async_copy(own_ref, out_ref.at[me], own_sem)
    keep.start()
    pl.semaphore_wait(barrier, n - 1)

    def copy_of(i):
        return pltpu.make_async_remote_copy(
            src_ref=own_ref,
            dst_ref=out_ref.at[me],
            send_sem=send_sem.at[i],
            recv_sem=recv_sem.at[i],
            device_id=(lax.rem(me + i, n), tp),
            device_id_type=MESH,
        )

    def start(i, carry):
        copy_of(i).start()
        return carry

    def finish(i, carry):
        copy_of(i).wait()
        return carry

    lax.fori_loop(1, n, start, 0)
    keep.wait()
    lax.fori_loop(1, n, finish, 0)


def gather_sp(block):
    n = lax.axis_size("sp")
    return pl.pallas_call(
        functools.partial(gather_kernel, n),
        out_shape=jax.ShapeDtypeStruct((n,) + block.shape, block.dtype),
        in_specs=[pl.BlockSpec(memory_space=pltpu.VMEM)],
        out_specs=pl.BlockSpec(memory_space=pltpu.VMEM),
        scratch_shapes=[
            pltpu.SemaphoreType.DMA((n,)),
            pltpu.SemaphoreType.DMA((n,)),
            pltpu.SemaphoreType.DMA,
        ],
        compiler_params=pltpu.CompilerParams(collective_id=0, has_side_effects=True),
        cost_estimate=pl.CostEstimate(flops=0, bytes_accessed=1 << 24, transcendentals=0),
        name="gather_kv",
    )(block)


def wide(value):
    return value.astype(jnp.float32)


def experts_kernel(
    part, residual, gain_mix, gain_pre, gain_moe, tail, wg_hbm, wu_hbm, wd_hbm, out,
    wg, wu, wd, got, middle, rows, active, partial, core_in, summed, far_in, near_in,
    x_in, y_in, w_sem, part_s, part_r, y_s, y_r, x_s, x_r, z_s, z_r, q_s, q_r, c_s, c_r,
    rc_s, rc_r, e_s, e_r, f_s, f_r, l_s, l_r, rx_s, rx_r, ry_s, ry_r,
):
    sp = lax.axis_index("sp")
    tp = lax.axis_index("tp")
    z, x = sp // PAIR, lax.rem(sp, PAIR)
    y, c = tp // PAIR, lax.rem(tp, PAIR)
    ox, oy, oc = 1 - x, 1 - y, 1 - c
    zp, zm, zq = lax.rem(z + 1, RING), lax.rem(z + 3, RING), lax.rem(z + 2, RING)
    width = residual.shape[1]
    to_c = (sp, y * PAIR + oc)
    to_y = (sp, oy * PAIR + c)
    to_yc = (sp, oy * PAIR + oc)
    to_x = (z * PAIR + ox, tp)
    to_zp = (zp * PAIR + x, tp)
    to_zm = (zm * PAIR + x, tp)
    peers = (to_c, to_y, to_yc, to_x, to_zp, to_zm)

    loads = [
        pltpu.make_async_copy(a, b, w_sem.at[i])
        for i, (a, b) in enumerate(((wg_hbm, wg), (wu_hbm, wu), (wd_hbm, wd)))
    ]
    for load in loads:
        load.start()
    barrier = pltpu.get_barrier_semaphore()
    for peer in peers:
        pl.semaphore_signal(barrier, inc=1, device_id=peer, device_id_type=MESH)
    pl.semaphore_wait(barrier, len(peers))

    started = []

    def send(src, dst, s, r, to):
        copy = pltpu.make_async_remote_copy(
            src_ref=src, dst_ref=dst, send_sem=s, recv_sem=r, device_id=to, device_id_type=MESH
        )
        copy.start()
        started.append(copy)
        return copy

    with jax.named_scope("proj"):
        copies = [
            send(part.at[to[1]], core_in.at[0, i], part_s.at[i], part_r.at[i], to)
            for i, to in ((2, to_yc), (1, to_y), (0, to_c))
        ]
        for copy in copies:
            copy.wait_recv()
        projected = wide(part[tp])
        for i in range(3):
            projected = projected + wide(core_in[0, i])
        mid = wide(residual[...]) + scale_rows(projected, gain_mix[...])
        middle[...] = mid
        mine = x * PAIR + y
        got[z, c, mine, :, 0:width] = scale_rows(mid, gain_pre[...]).astype(jnp.bfloat16)
        got[z, c, mine, :, width:] = tail[...]

    blk = (mine, x * PAIR + oy, ox * PAIR + y, ox * PAIR + oy)
    groups = (z, zm, zp, zq)

    def block(g, k):
        return got.at[groups[g], c, blk[k]]

    def relay(g, k):
        return send(block(g, k), block(g, k), c_s.at[g, k], c_r.at[g, k], to_c)

    relays = [[None] * 4 for _ in range(4)]
    plus, minus = [None] * 4, [None] * 4
    far = [None] * 4

    def spread(k):
        plus[k] = send(block(0, k), block(0, k), z_s.at[0, k], z_r.at[0, k], to_zp)
        minus[k] = send(block(0, k), block(0, k), z_s.at[1, k], z_r.at[1, k], to_zm)
        relays[0][k] = relay(0, k)

    with jax.named_scope("spread"):
        ycopy = send(block(0, 0), block(0, 0), y_s.at[0], y_r.at[0], to_y)
        xcopy0 = send(block(0, 0), block(0, 0), x_s.at[0], x_r.at[0], to_x)
        spread(0)
        ycopy.wait_recv()
        xcopy1 = send(block(0, 1), block(0, 1), x_s.at[1], x_r.at[1], to_x)
        spread(1)
        xcopy0.wait_recv()
        spread(2)
        xcopy1.wait_recv()
        spread(3)

    per = got.shape[2] * got.shape[3]

    def serve(g):
        group = groups[g]
        arrived = got[group].reshape(2 * per, got.shape[4])
        rows[...] = arrived
        spread_w = wide(rows[:, width:])
        lane = lax.broadcasted_iota(jnp.int32, spread_w.shape, 1)
        chosen = lax.rem(lane, spread_w.shape[1] // 2) == sp
        coef = jnp.sum(jnp.where(chosen, spread_w, 0.0), axis=1, keepdims=True)
        step = min(wg.shape[1], 256)

        @pl.loop(0, wg.shape[1] // step)
        def _(i):
            cols = pl.ds(pl.multiple_of(i * step, step), step)
            gate = jnp.dot(rows[:, 0:width], wg[:, cols], preferred_element_type=jnp.float32)
            up = jnp.dot(rows[:, 0:width], wu[:, cols], preferred_element_type=jnp.float32)
            gate = jnp.minimum(gate, clamp_limit)
            up = jnp.clip(up, -clamp_limit, clamp_limit)
            active[:, cols] = (gate * jax.nn.sigmoid(swish_alpha * gate) * (up + 1.0)).astype(
                jnp.bfloat16
            )

        @pl.loop(0, width // 512)
        def _(i):
            cols = pl.ds(pl.multiple_of(i * 512, 512), 512)
            down = jnp.dot(active[...], wd[:, cols], preferred_element_type=jnp.float32)
            partial[g, :, :, :, cols] = (
                (down * coef).astype(jnp.bfloat16).reshape(partial.shape[1:4] + (512,))
            )

        return send(partial.at[g, oc], core_in.at[g], rc_s.at[g], rc_r.at[g], to_c)

    def fold(g, copy):
        copy.wait_recv()
        for k in range(4):
            summed[g, k] = (wide(partial[g, c, k]) + wide(core_in[g, k])).astype(jnp.bfloat16)

    def await_core(g):
        for k in range(4):
            relays[g][k].wait_recv()

    half_a, half_b = pl.ds(x * PAIR, PAIR), pl.ds(ox * PAIR, PAIR)

    for load in loads:
        load.wait()
    with jax.named_scope("own"):
        await_core(0)
        back0 = serve(0)
    with jax.named_scope("near"):
        for k in range(4):
            plus[k].wait_recv()
            if k < 2:
                far[k] = send(block(1, k), block(1, k), q_s.at[k], q_r.at[k], to_zp)
            relays[1][k] = relay(1, k)
            minus[k].wait_recv()
            if k >= 2:
                far[k] = send(block(2, k), block(2, k), q_s.at[k], q_r.at[k], to_zm)
            relays[2][k] = relay(2, k)
        await_core(1)
        back1 = serve(1)
        fold(0, back0)
        for k in range(4):
            far[k].wait_recv()
            relays[3][k] = relay(3, k)
        await_core(2)
        back2 = serve(2)
        fold(1, back1)
        early_m = send(
            summed.at[1, half_a], near_in.at[1, half_a], e_s.at[1], e_r.at[1], to_zm
        )
    with jax.named_scope("far"):
        await_core(3)
        back3 = serve(3)
        fold(2, back2)
        early_p = send(
            summed.at[2, half_b], near_in.at[0, half_b], e_s.at[0], e_r.at[0], to_zp
        )
        fold(3, back3)
        far_p = send(summed.at[3, half_a], far_in.at[0], f_s.at[0], f_r.at[0], to_zp)
        far_m = send(summed.at[3, half_b], far_in.at[1], f_s.at[1], f_r.at[1], to_zm)
    with jax.named_scope("back"):
        far_p.wait_recv()
        for k in range(2):
            place = x * PAIR + k
            summed[2, place] = (wide(summed[2, place]) + wide(far_in[0, k])).astype(jnp.bfloat16)
        late_p = send(
            summed.at[2, half_a], near_in.at[0, half_a], l_s.at[0], l_r.at[0], to_zp
        )
        far_m.wait_recv()
        for k in range(2):
            place = ox * PAIR + k
            summed[1, place] = (wide(summed[1, place]) + wide(far_in[1, k])).astype(jnp.bfloat16)
        late_m = send(
            summed.at[1, half_b], near_in.at[1, half_b], l_s.at[1], l_r.at[1], to_zm
        )

        def total(place):
            return wide(summed[0, place]) + wide(near_in[0, place]) + wide(near_in[1, place])

        early_p.wait_recv()
        early_m.wait_recv()
        late_m.wait_recv()
        late_p.wait_recv()
        for k in range(2):
            place = ox * PAIR + k
            summed[0, place] = total(place).astype(jnp.bfloat16)
        xback = send(summed.at[0, half_b], x_in, rx_s.at[0], rx_r.at[0], to_x)
        xback.wait_recv()
        summed[0, blk[1]] = (total(blk[1]) + wide(x_in[oy])).astype(jnp.bfloat16)
        yback = send(summed.at[0, blk[1]], y_in, ry_s.at[0], ry_r.at[0], to_y)
        keep = total(mine) + wide(x_in[y])
        yback.wait_recv()
        mixture = keep + wide(y_in[...])
        out[...] = (middle[...] + scale_rows(mixture, gain_moe[...])).astype(out.dtype)
        for copy in started:
            copy.wait_send()


def experts_layer(part, residual, gain_mix, gain_pre, gain_moe, tail, w_gate, w_up, w_down):
    tok, width = residual.shape
    ff = w_gate.shape[1]
    full = width + tail.shape[1]
    blocks = PAIR * PAIR
    bf, f32 = jnp.bfloat16, jnp.float32
    dma = pltpu.SemaphoreType.DMA
    here = pl.BlockSpec(memory_space=pltpu.VMEM)
    there = pl.BlockSpec(memory_space=pl.ANY)
    sems = []
    for dims in (
        (3,), (1,), (2,), (2, 4), (4,), (4, 4), (4,), (2,), (2,), (2,), (1,), (1,)
    ):
        sems += [dma(dims), dma(dims)]
    return pl.pallas_call(
        experts_kernel,
        out_shape=jax.ShapeDtypeStruct((tok, width), bf),
        in_specs=[here] * 6 + [there] * 3,
        out_specs=here,
        scratch_shapes=[
            pltpu.VMEM((width, ff), bf),
            pltpu.VMEM((width, ff), bf),
            pltpu.VMEM((ff, width), bf),
            pltpu.VMEM((RING, PAIR, blocks, tok, full), bf),
            pltpu.VMEM((tok, width), f32),
            pltpu.VMEM((PAIR * blocks * tok, full), bf),
            pltpu.VMEM((PAIR * blocks * tok, ff), bf),
            pltpu.VMEM((RING, PAIR, blocks, tok, width), bf),
            pltpu.VMEM((RING, blocks, tok, width), bf),
            pltpu.VMEM((RING, blocks, tok, width), bf),
            pltpu.VMEM((2, PAIR, tok, width), bf),
            pltpu.VMEM((2, blocks, tok, width), bf),
            pltpu.VMEM((PAIR, tok, width), bf),
            pltpu.VMEM((tok, width), bf),
            dma((3,)),
        ]
        + sems,
        compiler_params=pltpu.CompilerParams(
            collective_id=1, has_side_effects=True, vmem_limit_bytes=56 << 20
        ),
        name="experts_layer",
    )(part, residual, gain_mix, gain_pre, gain_moe, tail, w_gate, w_up, w_down)


def weight_tail(routes, route_weights, experts):
    hits = routes[:, :, None] == jnp.arange(experts, dtype=jnp.int32)[None, None, :]
    coef = jnp.sum(jnp.where(hits, route_weights[:, :, None], 0.0), axis=1)
    high = lax.reduce_precision(coef, 8, 7)
    low = coef - high
    gap = jnp.zeros((coef.shape[0], LANES // 2 - experts), jnp.float32)
    return jnp.concatenate([high, gap, low, gap], axis=1).astype(jnp.bfloat16)


def on_device(
    queries,
    keys,
    values,
    q_gain,
    k_gain,
    w_out,
    residual,
    gain_mix,
    gain_pre,
    routes,
    route_weights,
    w_gate,
    w_up,
    w_down,
    gain_moe,
):
    tok_rows, head_local, head_size = queries.shape
    kv_local = keys.shape[1]
    group_size = head_local // kv_local
    positions = lax.axis_index("sp") * tok_rows + jnp.arange(tok_rows, dtype=jnp.int32)
    cosine_table, sine_table = rope_tables(positions, head_size)
    q_turned = (
        turn(scale_rows(queries.astype(jnp.float32), q_gain), cosine_table, sine_table)
        * head_size ** (-0.5)
    ).astype(jnp.bfloat16)
    k_turned = turn(scale_rows(keys.astype(jnp.float32), k_gain), cosine_table, sine_table).astype(
        jnp.bfloat16
    )
    q_grouped = q_turned.reshape(tok_rows, kv_local, group_size, head_size)
    initial = (
        jnp.full((kv_local, group_size, tok_rows), -jnp.inf, jnp.float32),
        jnp.zeros((kv_local, group_size, tok_rows), jnp.float32),
        jnp.zeros((kv_local, group_size, tok_rows, head_size), jnp.float32),
    )
    carry_state = initial
    kv_cols = kv_local * head_size
    both = gather_sp(
        jnp.concatenate(
            [k_turned.reshape(tok_rows, kv_cols), values.reshape(tok_rows, kv_cols)], axis=1
        )
    ).reshape(-1, 2 * kv_cols)
    key_piece = both[:, :kv_cols].reshape(-1, kv_local, head_size)
    value_piece = both[:, kv_cols:].reshape(-1, kv_local, head_size)
    piece_rows = key_piece.shape[0]
    block_rows = math.gcd(piece_rows, 1024)
    key_blocks = key_piece.reshape(piece_rows // block_rows, block_rows, kv_local, head_size)
    value_blocks = value_piece.reshape(piece_rows // block_rows, block_rows, kv_local, head_size)

    def absorb_block(state_now, key_value):
        running_max, running_sum, weighted = state_now
        key_block, value_block = key_value
        scores = jnp.einsum(
            "qkgd,skd->kgqs", q_grouped, key_block, preferred_element_type=jnp.float32
        )
        new_max = jnp.maximum(running_max, jnp.max(scores, axis=-1))
        rescale = jnp.exp(running_max - new_max)
        unnorm = jnp.exp(scores - new_max[..., None])
        running_sum = running_sum * rescale + jnp.sum(unnorm, axis=-1)
        weighted = weighted * rescale[..., None] + jnp.einsum(
            "kgqs,skd->kgqd",
            unnorm.astype(jnp.bfloat16),
            value_block,
            preferred_element_type=jnp.float32,
        )
        return ((new_max, running_sum, weighted), None)

    carry_state, ignored = lax.scan(absorb_block, carry_state, (key_blocks, value_blocks))
    running_max, running_sum, weighted = carry_state
    mixed_heads = (weighted / running_sum[..., None]).transpose(2, 0, 1, 3)
    mixed_heads = mixed_heads.reshape(tok_rows, head_local * head_size).astype(jnp.bfloat16)
    tok_part = residual.shape[0]
    width = residual.shape[1]
    part = jnp.dot(mixed_heads, w_out, preferred_element_type=jnp.float32).astype(jnp.bfloat16)
    local_experts = w_gate.shape[0]
    experts_all = local_experts * lax.axis_size("sp")
    capacity = max(2, (2 * tok_part * TOP + experts_all - 1) // experts_all)
    grid_fits = lax.axis_size("sp") == RING * PAIR and lax.axis_size("tp") == PAIR * PAIR
    if grid_fits and local_experts == 1 and capacity >= tok_part:
        return experts_layer(
            part.reshape(PAIR * PAIR, tok_part, width),
            residual,
            gain_mix[None],
            gain_pre[None],
            gain_moe[None],
            weight_tail(routes, route_weights, experts_all),
            w_gate[0],
            w_up[0],
            w_down[0],
        )
    projected = lax.psum_scatter(
        part,
        "tp",
        scatter_dimension=0,
        tiled=True,
    ).astype(jnp.float32)
    middle = residual.astype(jnp.float32) + scale_rows(projected, gain_mix)
    normed = scale_rows(middle, gain_pre).astype(jnp.bfloat16)
    tables = slot_table(routes, experts_all, capacity)
    chosen = jnp.sum(tables, axis=1)
    outbound = jnp.einsum("tp,td->pd", chosen, normed, preferred_element_type=jnp.float32)
    outbound = outbound.astype(jnp.bfloat16).reshape(experts_all, capacity, width)
    arrived_rows = lax.all_gather(
        lax.all_to_all(outbound, "sp", split_axis=0, concat_axis=0, tiled=True),
        "tp",
        axis=0,
        tiled=True,
    )
    leading = arrived_rows.shape[0] // local_experts
    partial_value = expert_apply(
        arrived_rows.reshape(leading, local_experts, arrived_rows.shape[1], width),
        w_gate,
        w_up,
        w_down,
    )
    summed = lax.psum_scatter(
        partial_value.reshape(arrived_rows.shape).astype(jnp.bfloat16),
        "tp",
        scatter_dimension=0,
        tiled=True,
    )
    returned = send_back(summed)
    gathered = jnp.einsum(
        "tkp,pd->tkd",
        tables,
        returned.reshape(experts_all * capacity, width),
        preferred_element_type=jnp.float32,
    )
    mixture = jnp.sum(gathered * route_weights[:, :, None], axis=1)
    return (middle + scale_rows(mixture, gain_moe)).astype(jnp.bfloat16)


def solution(mesh):
    placed = (
        P("sp", "tp", None),
        P("sp", "tp", None),
        P("sp", "tp", None),
        P(),
        P(),
        P("tp", None),
        P(("sp", "tp"), None),
        P(),
        P(),
        P(("sp", "tp"), None),
        P(("sp", "tp"), None),
        P("sp", None, "tp"),
        P("sp", None, "tp"),
        P("sp", "tp", None),
        P(),
    )
    return jax.shard_map(
        on_device, mesh=mesh, in_specs=placed, out_specs=P(("sp", "tp"), None), check_vma=False
    )
```

```python
import functools
import math

import jax
import jax.numpy as jnp
from jax import lax
from jax.experimental import pallas as pl
from jax.experimental.pallas import tpu as pltpu
from jax.sharding import PartitionSpec as P

TOP = 4
GRID_W = 64


norm_eps = 1e-06
rope_theta = 10000.0
clamp_limit = 7.0
swish_alpha = 1.702


def rope_tables(positions, head_size):
    row_index = (positions // GRID_W).astype(jnp.float32)
    col_index = (positions % GRID_W).astype(jnp.float32)
    freq_count = head_size // 4
    inverse = rope_theta ** (-jnp.arange(freq_count, dtype=jnp.float32) / freq_count)
    angles = jnp.stack([row_index[:, None] * inverse, col_index[:, None] * inverse], axis=1)
    return (jnp.cos(angles), jnp.sin(angles))


def turn(array_in, cosine_table, sine_table):
    token_count, head_count, head_size = array_in.shape
    split_field = array_in.reshape(token_count, head_count, 2, 2, head_size // 4)
    first_half = split_field[:, :, :, 0, :]
    second_half = split_field[:, :, :, 1, :]
    cos_wide = cosine_table[:, None]
    sin_wide = sine_table[:, None]
    turned = jnp.stack(
        [
            first_half * cos_wide - second_half * sin_wide,
            second_half * cos_wide + first_half * sin_wide,
        ],
        axis=3,
    )
    return turned.reshape(token_count, head_count, head_size)


def scale_rows(array_in, gain_vec):
    return (
        array_in
        * lax.rsqrt(jnp.mean(array_in * array_in, axis=-1, keepdims=True) + norm_eps)
        * gain_vec
    )


def slot_table(route_rows, experts, capacity):
    flat_routes = route_rows.reshape(-1)
    expert_hits = (flat_routes[:, None] == jnp.arange(experts, dtype=jnp.int32)[None, :]).astype(
        jnp.int32
    )
    slot_index = jnp.sum((jnp.cumsum(expert_hits, axis=0) - expert_hits) * expert_hits, axis=1)
    target = flat_routes * capacity + slot_index
    slot_onehot = target[:, None] == jnp.arange(experts * capacity, dtype=jnp.int32)[None, :]
    return slot_onehot.astype(jnp.bfloat16).reshape(
        route_rows.shape[0], route_rows.shape[1], experts * capacity
    )


def expert_apply(arrived_rows, w_gate, w_up, w_down):
    gate_pre = jnp.minimum(
        jnp.einsum("serd,edf->serf", arrived_rows, w_gate, preferred_element_type=jnp.float32),
        clamp_limit,
    )
    up_pre = jnp.clip(
        jnp.einsum("serd,edf->serf", arrived_rows, w_up, preferred_element_type=jnp.float32),
        -clamp_limit,
        clamp_limit,
    )
    active = (gate_pre * jax.nn.sigmoid(swish_alpha * gate_pre) * (up_pre + 1.0)).astype(
        jnp.bfloat16
    )
    partial_value = jnp.einsum("serf,efd->serd", active, w_down, preferred_element_type=jnp.float32)
    return lax.optimization_barrier(partial_value.astype(jnp.bfloat16)).astype(jnp.float32)


def send_back(finished):
    return lax.all_to_all(finished, "sp", split_axis=0, concat_axis=0, tiled=True)


MESH = pl.DeviceIdType.MESH
RING = 4
PAIR = 2
LANES = 128


def gather_kernel(n, own_ref, out_ref, send_sem, recv_sem, pass_sem, take_sem, own_sem):
    me = lax.axis_index("sp")
    tp = lax.axis_index("tp")
    pair = me + 1 - 2 * lax.rem(me, 2)
    barrier = pltpu.get_barrier_semaphore()

    def greet(i, carry):
        pl.semaphore_signal(
            barrier, inc=1, device_id=(lax.rem(me + 2 * i, n), tp), device_id_type=MESH
        )
        return carry

    lax.fori_loop(1, n // 2, greet, 0)
    pl.semaphore_signal(barrier, inc=1, device_id=(pair, tp), device_id_type=MESH)
    keep = pltpu.make_async_copy(own_ref, out_ref.at[me], own_sem)
    keep.start()
    pl.semaphore_wait(barrier, n // 2)

    def along(i):
        return pltpu.make_async_remote_copy(
            src_ref=own_ref,
            dst_ref=out_ref.at[me],
            send_sem=send_sem.at[i],
            recv_sem=recv_sem.at[i],
            device_id=(lax.rem(me + 2 * i, n), tp),
            device_id_type=MESH,
        )

    def across(i, src):
        return pltpu.make_async_remote_copy(
            src_ref=src,
            dst_ref=out_ref.at[lax.rem(me + n - 2 * i, n)],
            send_sem=pass_sem.at[i],
            recv_sem=take_sem.at[i],
            device_id=(pair, tp),
            device_id_type=MESH,
        )

    def relay(i):
        return across(i, out_ref.at[lax.rem(me + n - 2 * i, n)])

    def start(i, carry):
        along(i).start()
        return carry

    def forward(i, carry):
        along(i).wait_recv()
        relay(i).start()
        return carry

    def finish(i, carry):
        along(i).wait_send()
        relay(i).wait()
        return carry

    lax.fori_loop(1, n // 2, start, 0)
    across(0, own_ref).start()
    keep.wait()
    lax.fori_loop(1, n // 2, forward, 0)
    across(0, own_ref).wait()
    lax.fori_loop(1, n // 2, finish, 0)


def gather_sp(block):
    n = lax.axis_size("sp")
    return pl.pallas_call(
        functools.partial(gather_kernel, n),
        out_shape=jax.ShapeDtypeStruct((n,) + block.shape, block.dtype),
        in_specs=[pl.BlockSpec(memory_space=pltpu.VMEM)],
        out_specs=pl.BlockSpec(memory_space=pltpu.VMEM),
        scratch_shapes=[
            pltpu.SemaphoreType.DMA((n // 2,)),
            pltpu.SemaphoreType.DMA((n // 2,)),
            pltpu.SemaphoreType.DMA((n // 2,)),
            pltpu.SemaphoreType.DMA((n // 2,)),
            pltpu.SemaphoreType.DMA,
        ],
        compiler_params=pltpu.CompilerParams(collective_id=0, has_side_effects=True),
        cost_estimate=pl.CostEstimate(flops=0, bytes_accessed=1 << 24, transcendentals=0),
        name="gather_kv",
    )(block)


def wide(value):
    return value.astype(jnp.float32)


def experts_kernel(
    part, residual, gain_mix, gain_pre, gain_moe, tail, wg_hbm, wu_hbm, wd_hbm, out,
    wg, wu, wd, got, middle, rows, active, partial, core_in, summed, far_in, near_in,
    x_in, y_in, w_sem, part_s, part_r, y_s, y_r, x_s, x_r, z_s, z_r, q_s, q_r, c_s, c_r,
    rc_s, rc_r, e_s, e_r, f_s, f_r, l_s, l_r, rx_s, rx_r, ry_s, ry_r,
):
    sp = lax.axis_index("sp")
    tp = lax.axis_index("tp")
    z, x = sp // PAIR, lax.rem(sp, PAIR)
    y, c = tp // PAIR, lax.rem(tp, PAIR)
    ox, oy, oc = 1 - x, 1 - y, 1 - c
    zp, zm, zq = lax.rem(z + 1, RING), lax.rem(z + 3, RING), lax.rem(z + 2, RING)
    width = residual.shape[1]
    to_c = (sp, y * PAIR + oc)
    to_y = (sp, oy * PAIR + c)
    to_yc = (sp, oy * PAIR + oc)
    to_x = (z * PAIR + ox, tp)
    to_zp = (zp * PAIR + x, tp)
    to_zm = (zm * PAIR + x, tp)
    peers = (to_c, to_y, to_yc, to_x, to_zp, to_zm)

    loads = [
        pltpu.make_async_copy(a, b, w_sem.at[i])
        for i, (a, b) in enumerate(((wg_hbm, wg), (wu_hbm, wu), (wd_hbm, wd)))
    ]
    for load in loads:
        load.start()
    barrier = pltpu.get_barrier_semaphore()
    for peer in peers:
        pl.semaphore_signal(barrier, inc=1, device_id=peer, device_id_type=MESH)
    pl.semaphore_wait(barrier, len(peers))

    started = []

    def send(src, dst, s, r, to):
        copy = pltpu.make_async_remote_copy(
            src_ref=src, dst_ref=dst, send_sem=s, recv_sem=r, device_id=to, device_id_type=MESH
        )
        copy.start()
        started.append(copy)
        return copy

    with jax.named_scope("proj"):
        copies = [
            send(part.at[to[1]], core_in.at[0, i], part_s.at[i], part_r.at[i], to)
            for i, to in ((2, to_yc), (1, to_y), (0, to_c))
        ]
        for copy in copies:
            copy.wait_recv()
        projected = wide(part[tp])
        for i in range(3):
            projected = projected + wide(core_in[0, i])
        mid = wide(residual[...]) + scale_rows(projected, gain_mix[...])
        middle[...] = mid
        mine = x * PAIR + y
        got[z, c, mine, :, 0:width] = scale_rows(mid, gain_pre[...]).astype(jnp.bfloat16)
        got[z, c, mine, :, width:] = tail[...]

    blk = (mine, x * PAIR + oy, ox * PAIR + y, ox * PAIR + oy)
    groups = (z, zm, zp, zq)

    def block(g, k):
        return got.at[groups[g], c, blk[k]]

    def relay(g, k):
        return send(block(g, k), block(g, k), c_s.at[g, k], c_r.at[g, k], to_c)

    relays = [[None] * 4 for _ in range(4)]
    plus, minus = [None] * 4, [None] * 4
    far = [None] * 4

    def spread(k):
        plus[k] = send(block(0, k), block(0, k), z_s.at[0, k], z_r.at[0, k], to_zp)
        minus[k] = send(block(0, k), block(0, k), z_s.at[1, k], z_r.at[1, k], to_zm)
        relays[0][k] = relay(0, k)

    with jax.named_scope("spread"):
        ycopy = send(block(0, 0), block(0, 0), y_s.at[0], y_r.at[0], to_y)
        xcopy0 = send(block(0, 0), block(0, 0), x_s.at[0], x_r.at[0], to_x)
        spread(0)
        ycopy.wait_recv()
        xcopy1 = send(block(0, 1), block(0, 1), x_s.at[1], x_r.at[1], to_x)
        spread(1)
        xcopy0.wait_recv()
        spread(2)
        xcopy1.wait_recv()
        spread(3)

    per = got.shape[2] * got.shape[3]

    def serve(g):
        group = groups[g]
        arrived = got[group].reshape(2 * per, got.shape[4])
        rows[...] = arrived
        spread_w = wide(rows[:, width:])
        lane = lax.broadcasted_iota(jnp.int32, spread_w.shape, 1)
        chosen = lax.rem(lane, spread_w.shape[1] // 2) == sp
        coef = jnp.sum(jnp.where(chosen, spread_w, 0.0), axis=1, keepdims=True)
        step = min(wg.shape[1], 256)

        @pl.loop(0, wg.shape[1] // step)
        def _(i):
            cols = pl.ds(pl.multiple_of(i * step, step), step)
            gate = jnp.dot(rows[:, 0:width], wg[:, cols], preferred_element_type=jnp.float32)
            up = jnp.dot(rows[:, 0:width], wu[:, cols], preferred_element_type=jnp.float32)
            gate = jnp.minimum(gate, clamp_limit)
            up = jnp.clip(up, -clamp_limit, clamp_limit)
            active[:, cols] = (gate * jax.nn.sigmoid(swish_alpha * gate) * (up + 1.0)).astype(
                jnp.bfloat16
            )

        @pl.loop(0, width // 512)
        def _(i):
            cols = pl.ds(pl.multiple_of(i * 512, 512), 512)
            down = jnp.dot(active[...], wd[:, cols], preferred_element_type=jnp.float32)
            partial[g, :, :, :, cols] = (
                (down * coef).astype(jnp.bfloat16).reshape(partial.shape[1:4] + (512,))
            )

        return send(partial.at[g, oc], core_in.at[g], rc_s.at[g], rc_r.at[g], to_c)

    def fold(g, copy):
        copy.wait_recv()
        for k in range(4):
            summed[g, k] = (wide(partial[g, c, k]) + wide(core_in[g, k])).astype(jnp.bfloat16)

    def await_core(g):
        for k in range(4):
            relays[g][k].wait_recv()

    half_a, half_b = pl.ds(x * PAIR, PAIR), pl.ds(ox * PAIR, PAIR)

    for load in loads:
        load.wait()
    with jax.named_scope("own"):
        await_core(0)
        back0 = serve(0)
    with jax.named_scope("near"):
        for k in range(4):
            plus[k].wait_recv()
            if k < 2:
                far[k] = send(block(1, k), block(1, k), q_s.at[k], q_r.at[k], to_zp)
            relays[1][k] = relay(1, k)
            minus[k].wait_recv()
            if k >= 2:
                far[k] = send(block(2, k), block(2, k), q_s.at[k], q_r.at[k], to_zm)
            relays[2][k] = relay(2, k)
        await_core(1)
        back1 = serve(1)
        fold(0, back0)
        for k in range(4):
            far[k].wait_recv()
            relays[3][k] = relay(3, k)
        await_core(2)
        back2 = serve(2)
        fold(1, back1)
        early_m = send(
            summed.at[1, half_a], near_in.at[1, half_a], e_s.at[1], e_r.at[1], to_zm
        )
    with jax.named_scope("far"):
        await_core(3)
        back3 = serve(3)
        fold(2, back2)
        early_p = send(
            summed.at[2, half_b], near_in.at[0, half_b], e_s.at[0], e_r.at[0], to_zp
        )
        fold(3, back3)
        far_p = send(summed.at[3, half_a], far_in.at[0], f_s.at[0], f_r.at[0], to_zp)
        far_m = send(summed.at[3, half_b], far_in.at[1], f_s.at[1], f_r.at[1], to_zm)
    with jax.named_scope("back"):
        far_p.wait_recv()
        for k in range(2):
            place = x * PAIR + k
            summed[2, place] = (wide(summed[2, place]) + wide(far_in[0, k])).astype(jnp.bfloat16)
        late_p = send(
            summed.at[2, half_a], near_in.at[0, half_a], l_s.at[0], l_r.at[0], to_zp
        )
        far_m.wait_recv()
        for k in range(2):
            place = ox * PAIR + k
            summed[1, place] = (wide(summed[1, place]) + wide(far_in[1, k])).astype(jnp.bfloat16)
        late_m = send(
            summed.at[1, half_b], near_in.at[1, half_b], l_s.at[1], l_r.at[1], to_zm
        )

        def total(place):
            return wide(summed[0, place]) + wide(near_in[0, place]) + wide(near_in[1, place])

        early_p.wait_recv()
        early_m.wait_recv()
        late_m.wait_recv()
        late_p.wait_recv()
        for k in range(2):
            place = ox * PAIR + k
            summed[0, place] = total(place).astype(jnp.bfloat16)
        xback = send(summed.at[0, half_b], x_in, rx_s.at[0], rx_r.at[0], to_x)
        xback.wait_recv()
        summed[0, blk[1]] = (total(blk[1]) + wide(x_in[oy])).astype(jnp.bfloat16)
        yback = send(summed.at[0, blk[1]], y_in, ry_s.at[0], ry_r.at[0], to_y)
        keep = total(mine) + wide(x_in[y])
        yback.wait_recv()
        mixture = keep + wide(y_in[...])
        out[...] = (middle[...] + scale_rows(mixture, gain_moe[...])).astype(out.dtype)
        for copy in started:
            copy.wait_send()


def experts_layer(part, residual, gain_mix, gain_pre, gain_moe, tail, w_gate, w_up, w_down):
    tok, width = residual.shape
    ff = w_gate.shape[1]
    full = width + tail.shape[1]
    blocks = PAIR * PAIR
    bf, f32 = jnp.bfloat16, jnp.float32
    dma = pltpu.SemaphoreType.DMA
    here = pl.BlockSpec(memory_space=pltpu.VMEM)
    there = pl.BlockSpec(memory_space=pl.ANY)
    sems = []
    for dims in (
        (3,), (1,), (2,), (2, 4), (4,), (4, 4), (4,), (2,), (2,), (2,), (1,), (1,)
    ):
        sems += [dma(dims), dma(dims)]
    return pl.pallas_call(
        experts_kernel,
        out_shape=jax.ShapeDtypeStruct((tok, width), bf),
        in_specs=[here] * 6 + [there] * 3,
        out_specs=here,
        scratch_shapes=[
            pltpu.VMEM((width, ff), bf),
            pltpu.VMEM((width, ff), bf),
            pltpu.VMEM((ff, width), bf),
            pltpu.VMEM((RING, PAIR, blocks, tok, full), bf),
            pltpu.VMEM((tok, width), f32),
            pltpu.VMEM((PAIR * blocks * tok, full), bf),
            pltpu.VMEM((PAIR * blocks * tok, ff), bf),
            pltpu.VMEM((RING, PAIR, blocks, tok, width), bf),
            pltpu.VMEM((RING, blocks, tok, width), bf),
            pltpu.VMEM((RING, blocks, tok, width), bf),
            pltpu.VMEM((2, PAIR, tok, width), bf),
            pltpu.VMEM((2, blocks, tok, width), bf),
            pltpu.VMEM((PAIR, tok, width), bf),
            pltpu.VMEM((tok, width), bf),
            dma((3,)),
        ]
        + sems,
        compiler_params=pltpu.CompilerParams(
            collective_id=1, has_side_effects=True, vmem_limit_bytes=56 << 20
        ),
        name="experts_layer",
    )(part, residual, gain_mix, gain_pre, gain_moe, tail, w_gate, w_up, w_down)


def weight_tail(routes, route_weights, experts):
    hits = routes[:, :, None] == jnp.arange(experts, dtype=jnp.int32)[None, None, :]
    coef = jnp.sum(jnp.where(hits, route_weights[:, :, None], 0.0), axis=1)
    high = lax.reduce_precision(coef, 8, 7)
    low = coef - high
    gap = jnp.zeros((coef.shape[0], LANES // 2 - experts), jnp.float32)
    return jnp.concatenate([high, gap, low, gap], axis=1).astype(jnp.bfloat16)


def on_device(
    queries,
    keys,
    values,
    q_gain,
    k_gain,
    w_out,
    residual,
    gain_mix,
    gain_pre,
    routes,
    route_weights,
    w_gate,
    w_up,
    w_down,
    gain_moe,
):
    tok_rows, head_local, head_size = queries.shape
    kv_local = keys.shape[1]
    group_size = head_local // kv_local
    positions = lax.axis_index("sp") * tok_rows + jnp.arange(tok_rows, dtype=jnp.int32)
    cosine_table, sine_table = rope_tables(positions, head_size)
    q_turned = (
        turn(scale_rows(queries.astype(jnp.float32), q_gain), cosine_table, sine_table)
        * head_size ** (-0.5)
    ).astype(jnp.bfloat16)
    k_turned = turn(scale_rows(keys.astype(jnp.float32), k_gain), cosine_table, sine_table).astype(
        jnp.bfloat16
    )
    q_grouped = q_turned.reshape(tok_rows, kv_local, group_size, head_size)
    initial = (
        jnp.full((kv_local, group_size, tok_rows), -jnp.inf, jnp.float32),
        jnp.zeros((kv_local, group_size, tok_rows), jnp.float32),
        jnp.zeros((kv_local, group_size, tok_rows, head_size), jnp.float32),
    )
    carry_state = initial
    kv_cols = kv_local * head_size
    both = gather_sp(
        jnp.concatenate(
            [k_turned.reshape(tok_rows, kv_cols), values.reshape(tok_rows, kv_cols)], axis=1
        )
    ).reshape(-1, 2 * kv_cols)
    key_piece = both[:, :kv_cols].reshape(-1, kv_local, head_size)
    value_piece = both[:, kv_cols:].reshape(-1, kv_local, head_size)
    piece_rows = key_piece.shape[0]
    block_rows = math.gcd(piece_rows, 1024)
    key_blocks = key_piece.reshape(piece_rows // block_rows, block_rows, kv_local, head_size)
    value_blocks = value_piece.reshape(piece_rows // block_rows, block_rows, kv_local, head_size)

    def absorb_block(state_now, key_value):
        running_max, running_sum, weighted = state_now
        key_block, value_block = key_value
        scores = jnp.einsum(
            "qkgd,skd->kgqs", q_grouped, key_block, preferred_element_type=jnp.float32
        )
        new_max = jnp.maximum(running_max, jnp.max(scores, axis=-1))
        rescale = jnp.exp(running_max - new_max)
        unnorm = jnp.exp(scores - new_max[..., None])
        running_sum = running_sum * rescale + jnp.sum(unnorm, axis=-1)
        weighted = weighted * rescale[..., None] + jnp.einsum(
            "kgqs,skd->kgqd",
            unnorm.astype(jnp.bfloat16),
            value_block,
            preferred_element_type=jnp.float32,
        )
        return ((new_max, running_sum, weighted), None)

    carry_state, ignored = lax.scan(absorb_block, carry_state, (key_blocks, value_blocks))
    running_max, running_sum, weighted = carry_state
    mixed_heads = (weighted / running_sum[..., None]).transpose(2, 0, 1, 3)
    mixed_heads = mixed_heads.reshape(tok_rows, head_local * head_size).astype(jnp.bfloat16)
    tok_part = residual.shape[0]
    width = residual.shape[1]
    part = jnp.dot(mixed_heads, w_out, preferred_element_type=jnp.float32).astype(jnp.bfloat16)
    local_experts = w_gate.shape[0]
    experts_all = local_experts * lax.axis_size("sp")
    capacity = max(2, (2 * tok_part * TOP + experts_all - 1) // experts_all)
    grid_fits = lax.axis_size("sp") == RING * PAIR and lax.axis_size("tp") == PAIR * PAIR
    if grid_fits and local_experts == 1 and capacity >= tok_part:
        return experts_layer(
            part.reshape(PAIR * PAIR, tok_part, width),
            residual,
            gain_mix[None],
            gain_pre[None],
            gain_moe[None],
            weight_tail(routes, route_weights, experts_all),
            w_gate[0],
            w_up[0],
            w_down[0],
        )
    projected = lax.psum_scatter(
        part,
        "tp",
        scatter_dimension=0,
        tiled=True,
    ).astype(jnp.float32)
    middle = residual.astype(jnp.float32) + scale_rows(projected, gain_mix)
    normed = scale_rows(middle, gain_pre).astype(jnp.bfloat16)
    tables = slot_table(routes, experts_all, capacity)
    chosen = jnp.sum(tables, axis=1)
    outbound = jnp.einsum("tp,td->pd", chosen, normed, preferred_element_type=jnp.float32)
    outbound = outbound.astype(jnp.bfloat16).reshape(experts_all, capacity, width)
    arrived_rows = lax.all_gather(
        lax.all_to_all(outbound, "sp", split_axis=0, concat_axis=0, tiled=True),
        "tp",
        axis=0,
        tiled=True,
    )
    leading = arrived_rows.shape[0] // local_experts
    partial_value = expert_apply(
        arrived_rows.reshape(leading, local_experts, arrived_rows.shape[1], width),
        w_gate,
        w_up,
        w_down,
    )
    summed = lax.psum_scatter(
        partial_value.reshape(arrived_rows.shape).astype(jnp.bfloat16),
        "tp",
        scatter_dimension=0,
        tiled=True,
    )
    returned = send_back(summed)
    gathered = jnp.einsum(
        "tkp,pd->tkd",
        tables,
        returned.reshape(experts_all * capacity, width),
        preferred_element_type=jnp.float32,
    )
    mixture = jnp.sum(gathered * route_weights[:, :, None], axis=1)
    return (middle + scale_rows(mixture, gain_moe)).astype(jnp.bfloat16)


def solution(mesh):
    placed = (
        P("sp", "tp", None),
        P("sp", "tp", None),
        P("sp", "tp", None),
        P(),
        P(),
        P("tp", None),
        P(("sp", "tp"), None),
        P(),
        P(),
        P(("sp", "tp"), None),
        P(("sp", "tp"), None),
        P("sp", None, "tp"),
        P("sp", None, "tp"),
        P("sp", "tp", None),
        P(),
    )
    return jax.shard_map(
        on_device, mesh=mesh, in_specs=placed, out_specs=P(("sp", "tp"), None), check_vma=False
    )
```
